256 devices in a mesh: ep: 16 (over y, x), tp: 16 (over z, core).
Axes of the slice: x: 4, y: 4, z: 8, core: 2. Of those that a mesh axis runs over, the one named last changes fastest.
Arguments:
- scan_source_values: bfloat16 [1024, 32768], P('tp', 'ep'), may hold values from -6 to 6
- switch_path_values: bfloat16 [1024, 32768], P('tp', 'ep'), may hold values from -6 to 6
- causal_filter_coefficients: bfloat16 [1024, 4], replicated, may hold values from -3 to 3
- scan_switch_blockmap: bfloat16 [16, 64, 64], replicated, may hold values from -0.75 to 0.75
- entry_switch_blockmap: bfloat16 [16, 64, 64], replicated, may hold values from -0.75 to 0.75
- feature_fading_speeds: float32 [1024], replicated, may hold values from 0 to 1
- spike_amount: float32 [32768], P('ep'), may hold values from -1 to 0
- final_linear_map: bfloat16 [1024, 2048], replicated, may hold values from -0.1875 to 0.1875
- dispatched_group_activity: bfloat16 [32768, 2048], P(('ep', 'tp')), may hold values from -6 to 6
- specialist_rmsgain: bfloat16 [2048], replicated, may hold values from 0.099609375 to 1.8984375
- selected_specialist_ids: int32 [32768, 2], P(('ep', 'tp')), may hold values from 0 to 15, all different within a row; in each aligned block of 128 rows (0 to 127, 128 to 255, ...) at most 24 rows name the same one
- selected_specialist_share: float32 [32768, 2], P(('ep', 'tp')), may hold values from 0.2 to 1
- specialist_switch_maps: bfloat16 [16, 2048, 2048], P('ep', None, 'tp'), may hold values from -0.3125 to 0.3125
- specialist_widen_maps: bfloat16 [16, 2048, 2048], P('ep', None, 'tp'), may hold values from -0.3125 to 0.3125
- specialist_shrink_maps: bfloat16 [16, 2048, 2048], P('ep', None, 'tp'), may hold values from -0.03125 to 0.03125
Outputs:
- scan_path_result: bfloat16 [32768, 2048], P(('ep', 'tp'))
- moe_out: bfloat16 [32768, 2048], P(('ep', 'tp'))
The draws below stay inside these ranges and needn't reach their ends.
Inputs may be any that keep to these rules, and one draw needn't show every extreme that they name: `selected_specialist_ids`: each row names 2 different experts. Among the rows of one device no expert is named more than 24 times, and in every draw some device names some expert exactly 24 times.
All inputs are finite; a program needn't handle non-finite values.
Results may differ from the reference program's by a relative error of at most 0.0085.
Values may be sent and summed in bfloat16 or wider, within the bound.
A program may use at most 128 MiB of HBM per device.

```python
import math
import jax
import jax.numpy as jnp
import numpy as np
from jax import lax

D = 2048
WIDTH = 1024
BLOCK = 64
NBLK = 16
CONV = 4
FFE = 2048
TOPK = 2
EXPERTS = 16
TOK_A = 32768
MOE_DEV = 128
TOK_B = 32768
CAP = 24


def draw_feature_fading_speeds(key, part):
    first_key, second_key, third_key = jax.random.split(key, 3)
    slow_speed = jnp.exp(jax.random.uniform(first_key, (WIDTH,), jnp.float32, math.log(0.05), math.log(0.2))) / TOK_A
    fast_speed = jnp.exp(jax.random.uniform(second_key, (WIDTH,), jnp.float32, math.log(0.003), math.log(0.01)))
    fast_share = 0.5
    chosen = jax.random.uniform(third_key, (WIDTH,), jnp.float32) < fast_share
    return jnp.where(chosen, fast_speed, slow_speed)


def draw_spike_amount(key, part):
    first_key, second_key = jax.random.split(key)
    places = jax.random.randint(first_key, (8,), 0, TOK_A)
    depth = jnp.log(jax.random.uniform(second_key, (8,), jnp.float32, 0.5, 0.8))
    matches = (jnp.arange(TOK_A, dtype=jnp.int32)[:, None] == places[None, :]).astype(jnp.float32)
    return jnp.sum(matches * depth[None, :], axis=1)


def block_levels(rng, shape, cuts, least, largest):
    def one(dim, parts):
        heights = jax.random.uniform(jax.random.fold_in(jax.random.fold_in(rng, 6), dim), (parts,), jnp.float32, least / len(cuts), largest / len(cuts))
        return jnp.repeat(jnp.exp(heights), shape[dim] // parts).reshape((-1,) + (1,) * (len(shape) - dim - 1))

    gain = one(*cuts[0])
    for cut in cuts[1:]:
        gain = gain * one(*cut)
    return gain


def shared_out(own_key, own, number, rows, count, top, most, skew):
    sequence = jax.random.permutation(own_key, count)
    packed, ordinary = load_shares(count, rows * top, most, skew, True), load_shares(count, rows * top, most, skew, False)
    places = jnp.arange(count)

    def named(tallies, offset_by):
        used = int((tallies > 0).sum())
        fixed = max(1, used // 4)
        shifted = fixed + (places - fixed + offset_by * (used - fixed)) % max(1, count - fixed)
        return jnp.zeros((count,), jnp.int32).at[sequence[jnp.where(places < fixed, places, shifted)]].set(jnp.asarray(tallies, jnp.int32))

    tallies = jnp.where(number % 4 == 0, named(packed, number // 4), named(ordinary, number - number // 4 - 1))
    mixed = jax.random.permutation(jax.random.fold_in(own, 3), count)
    giver, receiver = mixed[0:count // 2 * 2:2], mixed[1:count // 2 * 2:2]
    margin = jnp.minimum(tallies[giver] - 1, most - tallies[receiver]) // 2
    margin = jnp.where((giver == sequence[0]) | (receiver == sequence[0]) | (tallies[receiver] == 0), 0, jnp.maximum(margin, 0))
    shifted = jax.random.randint(jax.random.fold_in(own, 4), (count // 2,), 0, 1 << 20) % (margin + 1)
    tallies = tallies.at[giver].add(-shifted).at[receiver].add(shifted)
    items = jnp.searchsorted(jnp.cumsum(tallies), jnp.arange(rows * top), side="right").astype(jnp.int32)
    table = items.reshape(top, rows).T
    table = table[jax.random.permutation(jax.random.fold_in(own, 1), rows)]
    offset_by = jax.random.randint(jax.random.fold_in(own, 2), (rows, 1), 0, top)
    return jnp.take_along_axis(table, (jnp.arange(top)[None, :] + offset_by) % top, axis=1)


def load_shares(count, total, most, slope, full):
    weights = [(1 << 20) // math.isqrt(grade ** slope) + 1 for grade in range(1, count + 1)]
    largest = most if full else min(most, max(-(-total // count), total * weights[0] // sum(weights)))
    least = 1 if total - largest >= count - 1 else 0
    holding, surplus = [largest] + [least] * (count - 1), total - largest - least * (count - 1)
    while surplus > 0:
        movable = [i for i in range(1, count) if holding[i] < largest] or [i for i in range(1, count) if holding[i] < most]
        whole, remaining = sum([weights[i] for i in movable]), surplus
        for i in movable:
            addition = min(most - holding[i], max(1, remaining * weights[i] // whole), surplus)
            holding[i] = holding[i] + addition
            surplus = surplus - addition
    return np.array(holding)


def noise(stream_key, shape, spread, bound, cuts=(), kind=jnp.bfloat16):
    loudness = block_levels(stream_key, shape, cuts, -0.22, 0.18) if cuts else 1.0
    array = jax.random.normal(stream_key, shape, jnp.float32) * spread * loudness
    return jnp.minimum(jnp.maximum(array, -bound), bound).astype(kind)


def setup_inputs(seed: int = 0) -> dict:
    streams_of = jax.random.split(jax.random.key(seed), 16)
    scan_source_values = noise(streams_of[0], (WIDTH, TOK_A), 1.0, 6.0, ((0, 16), (1, 16)))
    switch_path_values = noise(streams_of[1], (WIDTH, TOK_A), 1.0, 6.0, ((0, 16), (1, 16)))
    causal_filter_coefficients = noise(streams_of[2], (WIDTH, CONV), CONV ** -0.5, 3.0)
    scan_switch_blockmap = noise(streams_of[3], (NBLK, BLOCK, BLOCK), BLOCK ** -0.5, 0.75)
    entry_switch_blockmap = noise(streams_of[4], (NBLK, BLOCK, BLOCK), BLOCK ** -0.5, 0.75)
    feature_fading_speeds = draw_feature_fading_speeds(jax.random.fold_in(streams_of[15], 71), 0)
    spike_amount = draw_spike_amount(jax.random.fold_in(streams_of[15], 71), 0)
    final_linear_map = noise(streams_of[7], (WIDTH, D), WIDTH ** -0.5, 0.1875)
    dispatched_group_activity = noise(streams_of[8], (TOK_B, D), 1.0, 6.0, ((0, 256),))
    specialist_rmsgain = jnp.clip(1.0 + 0.18 * jax.random.normal(streams_of[9], (D,), jnp.float32), 0.099609375, 1.8984375).astype(jnp.bfloat16)
    selected_specialist_ids_keys = jax.random.split(jax.random.fold_in(streams_of[10], 1), TOK_B // MOE_DEV)
    selected_specialist_ids_turns = jax.random.permutation(jax.random.fold_in(streams_of[10], 3), TOK_B // MOE_DEV)
    selected_specialist_ids = jax.vmap(lambda own, number: shared_out(jax.random.fold_in(streams_of[10], 2), own, number, MOE_DEV, EXPERTS, TOPK, CAP, 2))(selected_specialist_ids_keys, selected_specialist_ids_turns).reshape((TOK_B, TOPK))
    selected_specialist_share = jnp.clip(0.2 + 0.8 * jax.random.uniform(streams_of[11], (TOK_B, TOPK), jnp.float32) ** block_levels(streams_of[11], (TOK_B, TOPK), ((0, 256),), -0.2, 0.2), 0.2, 1.0)
    specialist_switch_maps = noise(streams_of[12], (EXPERTS, D, FFE), (D // 6) ** -0.5, 0.3125, ((0, 16), (2, 16)))
    specialist_widen_maps = noise(streams_of[13], (EXPERTS, D, FFE), (D // 6) ** -0.5, 0.3125, ((0, 16), (2, 16)))
    specialist_shrink_maps = noise(streams_of[14], (EXPERTS, D, FFE), (16 * FFE) ** -0.5, 0.03125, ((0, 16), (2, 16)))
    return {"scan_source_values": scan_source_values, "switch_path_values": switch_path_values, "causal_filter_coefficients": causal_filter_coefficients, "scan_switch_blockmap": scan_switch_blockmap, "entry_switch_blockmap": entry_switch_blockmap, "feature_fading_speeds": feature_fading_speeds, "spike_amount": spike_amount, "final_linear_map": final_linear_map, "dispatched_group_activity": dispatched_group_activity, "specialist_rmsgain": specialist_rmsgain, "selected_specialist_ids": selected_specialist_ids, "selected_specialist_share": selected_specialist_share, "specialist_switch_maps": specialist_switch_maps, "specialist_widen_maps": specialist_widen_maps, "specialist_shrink_maps": specialist_shrink_maps}


def combine_pairs(earlier, later):
    return (earlier[0] * later[0], later[0] * earlier[1] + later[1])

def scan_path(scan_source_values, switch_path_values, causal_filter_coefficients, scan_switch_blockmap, entry_switch_blockmap, feature_fading_speeds, spike_amount, final_linear_map):
    positions = scan_source_values.shape[1]
    padded = jnp.pad(scan_source_values.astype(jnp.float32), ((0, 0), (CONV - 1, 0)))
    conv_taps = causal_filter_coefficients.astype(jnp.float32)
    running = padded[:, 0:positions] * conv_taps[:, 0:1]
    for shift_tap in range(1, CONV):
        running = running + padded[:, shift_tap:shift_tap + positions] * conv_taps[:, shift_tap:shift_tap + 1]
    conv_out = running.astype(jnp.bfloat16)
    grouped = conv_out.astype(jnp.float32).reshape(NBLK, BLOCK, positions)
    scan_switch = jax.nn.sigmoid(jnp.einsum('gij,git->gjt', scan_switch_blockmap.astype(jnp.float32), grouped).reshape(WIDTH, positions))
    inflow = jax.nn.sigmoid(jnp.einsum('gij,git->gjt', entry_switch_blockmap.astype(jnp.float32), grouped).reshape(WIDTH, positions))
    fading_exponent = -8.0 * scan_switch * feature_fading_speeds[:, None] + spike_amount[None, :]
    drive = jnp.sqrt(-jnp.expm1(2.0 * fading_exponent)) * inflow * conv_out.astype(jnp.float32)
    unused, state = lax.associative_scan(combine_pairs, (jnp.exp(fading_exponent), drive), axis=1)
    mix_hidden = (state * jax.nn.gelu(switch_path_values.astype(jnp.float32), approximate=True)).astype(jnp.bfloat16)
    return jnp.dot(mix_hidden.T, final_linear_map, preferred_element_type=jnp.float32).astype(jnp.bfloat16)

def expert_branch(dispatched_group_activity, specialist_rmsgain, selected_specialist_ids, selected_specialist_share, specialist_switch_maps, specialist_widen_maps, specialist_shrink_maps):
    values = dispatched_group_activity.astype(jnp.float32)
    scale = lax.rsqrt(lax.optimization_barrier(jnp.mean(values * values, axis=1, keepdims=True)) + 1e-06)
    normed = (values * scale * specialist_rmsgain.astype(jnp.float32)).astype(jnp.bfloat16)
    token_total, route_count = selected_specialist_ids.shape
    model_width = dispatched_group_activity.shape[1]
    block_count = token_total // MOE_DEV
    flat_ids = selected_specialist_ids.reshape(block_count, MOE_DEV * route_count)
    one_hot = (flat_ids[:, :, None] == jnp.arange(EXPERTS, dtype=jnp.int32)[None, None, :]).astype(jnp.int32)
    slot_rank = lax.optimization_barrier(jnp.sum((jnp.cumsum(one_hot, axis=1) - one_hot) * one_hot, axis=2))
    owner_token = jnp.arange(block_count, dtype=jnp.int32)[:, None] * MOE_DEV + jnp.arange(MOE_DEV * route_count, dtype=jnp.int32)[None, :] // route_count
    flat_weight = selected_specialist_share.reshape(block_count, MOE_DEV * route_count)
    padded_rows = jnp.concatenate([normed, jnp.zeros((1, model_width), jnp.bfloat16)], axis=0)
    slot_total = block_count * CAP

    def one_expert(running, expert):
        mine = flat_ids == expert
        slot_index = jnp.where(mine, jnp.arange(block_count, dtype=jnp.int32)[:, None] * CAP + slot_rank, slot_total).astype(jnp.int32)
        slot_token = jnp.full((slot_total + 1,), token_total, jnp.int32).at[slot_index.reshape(-1)].set(owner_token.reshape(-1))[:slot_total]
        slot_weight = jnp.zeros((slot_total + 1,), jnp.float32).at[slot_index.reshape(-1)].set(flat_weight.reshape(-1))[:slot_total]
        rows = padded_rows[jnp.minimum(slot_token, token_total)]
        gate_pre = jnp.dot(rows, specialist_switch_maps[expert], preferred_element_type=jnp.float32)
        up_pre = jnp.dot(rows, specialist_widen_maps[expert], preferred_element_type=jnp.float32)
        gate_cut = jnp.minimum(gate_pre, 7.0)
        up_cut = jnp.clip(up_pre, -7.0, 7.0)
        units = ((up_cut + 1.0) * gate_cut * jax.nn.sigmoid(1.702 * gate_cut)).astype(jnp.bfloat16)
        result = lax.dot_general(units, specialist_shrink_maps[expert], (((1,), (1,)), ((), ())), preferred_element_type=jnp.float32).astype(jnp.bfloat16)
        running = running.at[slot_token].add(result.astype(jnp.float32) * slot_weight[:, None], mode='drop')
        return (running, None)
    running, unused = lax.scan(one_expert, jnp.zeros((token_total, model_width), jnp.float32), jnp.arange(EXPERTS, dtype=jnp.int32))
    return running.astype(jnp.bfloat16)

def reference(scan_source_values, switch_path_values, causal_filter_coefficients, scan_switch_blockmap, entry_switch_blockmap, feature_fading_speeds, spike_amount, final_linear_map, dispatched_group_activity, specialist_rmsgain, selected_specialist_ids, selected_specialist_share, specialist_switch_maps, specialist_widen_maps, specialist_shrink_maps):
    scan_path_result = scan_path(scan_source_values, switch_path_values, causal_filter_coefficients, scan_switch_blockmap, entry_switch_blockmap, feature_fading_speeds, spike_amount, final_linear_map)
    moe_out = expert_branch(dispatched_group_activity, specialist_rmsgain, selected_specialist_ids, selected_specialist_share, specialist_switch_maps, specialist_widen_maps, specialist_shrink_maps)
    return (scan_path_result, moe_out)
```

```python
import functools

import jax
import jax.numpy as jnp
from jax import lax
from jax.experimental import pallas as pl
from jax.experimental.pallas import tpu as pltpu
from jax.sharding import PartitionSpec as P

MESH = pl.DeviceIdType.MESH
F32 = jnp.float32
BF16 = jnp.bfloat16
CAP = 24
ROWS = 384
DM = 2048
SHARD = 128
NZ = 8
NEP = 16
NDC = 4
DC = DM // NDC
NG = 4
GROWS = 1024
BLOCK = 64


def from_everyone(x, axis):
    copies = jnp.broadcast_to(x, (lax.axis_size(axis), *x.shape))
    return lax.all_to_all(copies, axis, split_axis=0, concat_axis=0, tiled=True)


def all_in_one(x, axis):
    leaves = jax.tree.leaves(x)
    sequence = sorted(range(len(leaves)), key=lambda k: -leaves[k].size)
    width = (1, *leaves[sequence[0]].shape)[-1]
    lines = [
        jnp.pad(leaves[k].reshape(-1), (0, -leaves[k].size % width)).reshape(-1, width)
        for k in sequence
    ]
    both, at, found = (from_everyone(jnp.concatenate(lines), axis), 0, {})
    for k, line in zip(sequence, lines):
        section = both[:, at : at + len(line)].reshape(len(both), -1)
        found[k] = section[:, : leaves[k].size].reshape(-1, *leaves[k].shape)
        at += len(line)
    numbers = iter(range(len(leaves)))
    return jax.tree.map(lambda _: found[next(numbers)], x)


def folded_in_pairs(pieces, combine):
    while len(jax.tree.leaves(pieces)[0]) > 1:
        pieces = jax.vmap(combine)(
            *(jax.tree.map(lambda part: part[side::2], pieces) for side in (0, 1))
        )
    return jax.tree.map(lambda part: part[0], pieces)


def prefix(x, axis, combine, identity):
    count, index = (lax.axis_size(axis), lax.axis_index(axis))
    passed = jnp.arange(count) < index

    def kept(part, zero, own):
        part = jnp.where(
            passed.reshape(-1, *(1 for _ in own.shape)), part, jnp.asarray(zero, own.dtype)
        )
        return part

    pieces = all_in_one(x, axis)
    return folded_in_pairs(jax.tree.map(kept, pieces, identity, x), combine)


def from_behind(x, axis, by):
    count = lax.axis_size(axis)
    pairs = [(i, i + by) for i in range(count) if 0 <= i + by < count]
    return lax.ppermute(x, axis, pairs)


def cut_along(x, dim, count):
    dims = x.shape
    blocks = x.reshape(*dims[:dim], count, dims[dim] // count, *dims[dim + 1 :])
    return jnp.moveaxis(blocks, dim, 0)


def cut_rows(length, count):
    hop = length // count
    if hop >= 8:
        hop -= hop % 8
    return [hop * k for k in range(1, count)]


def laid_out(blocks, dim):
    blocks = jnp.moveaxis(blocks, 0, dim)
    dims = blocks.shape
    return blocks.reshape(*dims[:dim], dims[dim] * dims[dim + 1], *dims[dim + 2 :])


def cut_exchange(x, axis, pieces, split_dim, concat_dim):
    blocks = cut_along(x, split_dim, lax.axis_size(axis))
    split_at = max(range(1, max(2, blocks.ndim - 1)), key=lambda d: blocks.shape[d])
    finished = []
    for section in jnp.split(blocks, cut_rows(blocks.shape[split_at], pieces), axis=split_at):
        if section.size:
            finished.append(lax.all_to_all(section, axis, split_axis=0, concat_axis=0, tiled=True))
    return laid_out(jnp.concatenate(finished, axis=split_at), concat_dim)


def combine_pairs(earlier, later):
    return (earlier[0] * later[0], later[0] * earlier[1] + later[1])


def segment_recurrence(decay, drive):
    channels, positions = decay.shape
    span = 16
    seg_count = positions // span
    decay_split = decay.reshape(channels, seg_count, span).transpose(0, 2, 1)
    drive_split = drive.reshape(channels, seg_count, span).transpose(0, 2, 1)
    run_state = jnp.zeros((channels, seg_count), jnp.float32)
    run_decay = jnp.ones((channels, seg_count), jnp.float32)
    state_list = []
    decay_list = []
    for offset in range(span):
        run_state = decay_split[:, offset] * run_state + drive_split[:, offset]
        run_decay = run_decay * decay_split[:, offset]
        state_list.append(run_state)
        decay_list.append(run_decay)
    local_state = jnp.stack(state_list, axis=1)
    local_decay = jnp.stack(decay_list, axis=1)
    decay_upto, state_upto = lax.associative_scan(combine_pairs, (run_decay, run_state), axis=1)
    decay_before = jnp.concatenate(
        [jnp.ones((channels, 1), jnp.float32), decay_upto[:, :-1]], axis=1
    )
    state_before = jnp.concatenate(
        [jnp.zeros((channels, 1), jnp.float32), state_upto[:, :-1]], axis=1
    )
    identity = (jnp.ones((channels,), jnp.float32), jnp.zeros((channels,), jnp.float32))
    carried = prefix((decay_upto[:, -1], state_upto[:, -1]), "ep", combine_pairs, identity)
    entering = state_before + decay_before * carried[1][:, None]
    state = local_state + local_decay * entering[:, None, :]
    return state.transpose(0, 2, 1).reshape(channels, positions)


def mixer_half(
    scan_source_values,
    switch_path_values,
    causal_filter_coefficients,
    scan_switch_blockmap,
    entry_switch_blockmap,
    feature_fading_speeds,
    spike_amount,
    final_linear_map,
):
    channels, positions = scan_source_values.shape
    tp_index = lax.axis_index("tp")
    first_chan = tp_index * channels
    conv_local = lax.dynamic_slice_in_dim(
        causal_filter_coefficients, first_chan, channels, 0
    ).astype(jnp.float32)
    tap_count = conv_local.shape[1]
    rim_cells = from_behind(scan_source_values[:, positions - tap_count + 1 :], "ep", 1)
    padded = jnp.concatenate([rim_cells, scan_source_values], axis=1).astype(jnp.float32)
    running = padded[:, 0:positions] * conv_local[:, 0:1]
    for shift_tap in range(1, tap_count):
        running = (
            running
            + padded[:, shift_tap : shift_tap + positions]
            * conv_local[:, shift_tap : shift_tap + 1]
        )
    conv_out = running.astype(jnp.bfloat16)
    block_count = channels // BLOCK
    rate_local = lax.dynamic_slice_in_dim(
        scan_switch_blockmap, tp_index * block_count, block_count, 0
    )
    input_local = lax.dynamic_slice_in_dim(
        entry_switch_blockmap, tp_index * block_count, block_count, 0
    )
    grouped = conv_out.reshape(block_count, BLOCK, positions)
    block_dims = (((1,), (1,)), ((0,), (0,)))
    scan_switch = jax.nn.sigmoid(
        lax.dot_general(
            rate_local, grouped, block_dims, preferred_element_type=jnp.float32
        ).reshape(channels, positions)
    )
    inflow = jax.nn.sigmoid(
        lax.dot_general(
            input_local, grouped, block_dims, preferred_element_type=jnp.float32
        ).reshape(channels, positions)
    )
    feature_fading = lax.dynamic_slice_in_dim(feature_fading_speeds, first_chan, channels, 0)
    fading_exponent = -8.0 * scan_switch * feature_fading[:, None] + spike_amount[None, :]
    drive = jnp.sqrt(-jnp.expm1(2.0 * fading_exponent)) * inflow * conv_out.astype(jnp.float32)
    state = segment_recurrence(jnp.exp(fading_exponent), drive)
    mix_hidden = (
        state * jax.nn.gelu(switch_path_values.astype(jnp.float32), approximate=True)
    ).astype(jnp.bfloat16)
    tp_count = lax.axis_size("tp")
    pieces = mix_hidden.reshape(channels, tp_count, positions // tp_count)
    return lax.dot_general(
        lax.all_to_all(pieces, "tp", split_axis=1, concat_axis=0, tiled=True)[:, 0, :],
        final_linear_map,
        (((0,), (0,)), ((), ())),
        preferred_element_type=jnp.float32,
    ).astype(jnp.bfloat16)


def expert_kernel(
    tok_ref, gain_ref, meta_ref, g_ref, u_ref, d_ref, out_ref,
    gbuf, ubuf, dbuf, snd, xin, xmat, units, acc, ps, pr, rs, rb, comb,
    ag_send, ag_recv, ds_send, ds_recv, xs_send, xs_recv, ps_send, ps_recv, rt_send, rt_recv,
):
    ep = lax.axis_index("ep")
    tp = lax.axis_index("tp")
    z = tp // 2
    core = lax.rem(tp, 2)
    sib = z * 2 + (1 - core)
    nbr = (lax.rem(z + 1, NZ) * 2 + core, lax.rem(z + NZ - 1, NZ) * 2 + core)

    bar = pltpu.get_barrier_semaphore()
    for who in (nbr[0], nbr[1], sib):
        pl.semaphore_signal(bar, inc=1, device_id=(ep, who), device_id_type=MESH)

    @pl.loop(1, NEP)
    def _(k):
        pl.semaphore_signal(bar, inc=1, device_id=(lax.rem(ep + k, NEP), tp), device_id_type=MESH)

    pl.semaphore_wait(bar, 3 + NEP - 1)

    def piece(p):
        if p < NG:
            return (g_ref, gbuf, (p % 2) * GROWS, GROWS) if p < 2 else (u_ref, ubuf, (p % 2) * GROWS, GROWS)
        return d_ref, dbuf, (p - NG) * DC, DC

    def ring(d, hop, p, origin):
        own, buf, lo, n = piece(p)
        last = isinstance(hop, int) and hop == 4
        if last:
            n = n // 2
            lo = lo + d * n
        first = isinstance(hop, int) and hop == 1
        src = own.at[pl.ds(lo, n)] if first else buf.at[origin, pl.ds(lo, n)]
        return pltpu.make_async_remote_copy(
            src_ref=src, dst_ref=buf.at[origin, pl.ds(lo, n)],
            send_sem=ag_send.at[d, hop - 1, p], recv_sem=ag_recv.at[d, hop - 1, p],
            device_id=(ep, nbr[d]), device_id_type=MESH,
        )

    def sent(d, hop):
        return lax.rem(z + NZ - (hop - 1), NZ) if d == 0 else lax.rem(z + hop - 1, NZ)

    def came(d, hop):
        return lax.rem(z + NZ - hop, NZ) if d == 0 else lax.rem(z + hop, NZ)

    def start(pieces, hop):
        for p in pieces:
            for d in (0, 1):
                ring(d, hop, p, sent(d, hop)).start()

    def forward(pieces, hop, last=False):
        for p in pieces:
            for d in (0, 1):
                ring(d, hop, p, came(d, hop)).wait_recv()
                nxt = 4 if last else hop + 1
                ring(d, nxt, p, sent(d, nxt)).start()

    def arrive(pieces):
        for p in pieces:
            for d in (0, 1):
                ring(d, 4, p, came(d, 4)).wait_recv()

    gu = list(range(NG))
    dn = list(range(NG, NG + NDC))
    start(gu, 1)

    gbuf[z] = g_ref[...]
    ubuf[z] = u_ref[...]
    dbuf[z] = d_ref[...]

    values = tok_ref[...].astype(F32)
    scale = lax.rsqrt(jnp.mean(values * values, axis=1, keepdims=True) + 1e-06)
    normed = (values * scale * gain_ref[...].astype(F32)).astype(BF16)
    expert_no = lax.broadcasted_iota(jnp.int32, (NEP, SHARD), 0).astype(F32)
    is0 = meta_ref[0:1, :] == expert_no
    is1 = meta_ref[1:2, :] == expert_no
    member = jnp.where(is0 | is1, 1.0, 0.0)
    weight = jnp.where(is0, meta_ref[2:3, :], 0.0) + jnp.where(is1, meta_ref[3:4, :], 0.0)
    before = (
        lax.broadcasted_iota(jnp.int32, (SHARD, SHARD), 0)
        < lax.broadcasted_iota(jnp.int32, (SHARD, SHARD), 1)
    )
    rank = jnp.dot(
        member.astype(BF16), jnp.where(before, 1.0, 0.0).astype(BF16), preferred_element_type=F32
    )
    place = jnp.where(member > 0.0, rank, -1.0)
    slot_no = lax.broadcasted_iota(jnp.int32, (CAP, SHARD), 0).astype(F32)
    picks, shares = [], []
    for e in range(NEP):
        hit = place[e : e + 1, :] == slot_no
        picks.append(jnp.where(hit, 1.0, 0.0))
        shares.append(jnp.where(hit, weight[e : e + 1, :], 0.0))
    pick = jnp.concatenate(picks, axis=0).astype(BF16)
    share = jnp.concatenate(shares, axis=0).T
    share_hi = share.astype(BF16)
    comb[0] = share_hi
    comb[1] = (share - share_hi.astype(F32)).astype(BF16)
    for k in range(4):
        rows = jnp.dot(pick, normed[:, k * 512 : (k + 1) * 512], preferred_element_type=F32)
        snd[:, :, k * 512 : (k + 1) * 512] = rows.reshape(NEP, CAP, 512).astype(BF16)

    def dispatch(peer, src):
        return pltpu.make_async_remote_copy(
            src_ref=snd.at[peer], dst_ref=xin.at[core, src],
            send_sem=ds_send.at[peer], recv_sem=ds_recv.at[src],
            device_id=(peer, tp), device_id_type=MESH,
        )

    @pl.loop(1, NEP)
    def _(k):
        dispatch(lax.rem(ep + k, NEP), ep).start()

    xin[core, ep] = snd[ep]

    forward(gu, 1)

    @pl.loop(1, NEP)
    def _(k):
        src = lax.rem(ep + k, NEP)
        dispatch(src, src).wait_recv()

    to_sib = pltpu.make_async_remote_copy(
        src_ref=xin.at[core], dst_ref=xin.at[core], send_sem=xs_send, recv_sem=xs_recv,
        device_id=(ep, sib), device_id_type=MESH,
    )
    from_sib = pltpu.make_async_remote_copy(
        src_ref=xin.at[1 - core], dst_ref=xin.at[1 - core], send_sem=xs_send, recv_sem=xs_recv,
        device_id=(ep, sib), device_id_type=MESH,
    )
    to_sib.start()
    from_sib.wait_recv()

    @pl.loop(0, 2 * (NEP // 2))
    def _(i):
        half = i // (NEP // 2)
        pair = lax.rem(i, NEP // 2)
        two = xin[half, pl.ds(pair * 2, 2)].astype(F32).reshape(2 * CAP, DM)
        xmat[half, pl.ds(pl.multiple_of(pair * 2 * CAP, 16), 2 * CAP), :] = two.astype(BF16)

    def hidden(origin):
        @pl.loop(0, 2)
        def _(half):
            both = jnp.concatenate([gbuf[origin], ubuf[origin]], axis=1)
            pre = jnp.dot(xmat[half], both, preferred_element_type=F32)
            gate = jnp.minimum(pre[:, :SHARD], 7.0)
            up = jnp.clip(pre[:, SHARD:], -7.0, 7.0)
            units[half, origin] = ((up + 1.0) * gate * jax.nn.sigmoid(1.702 * gate)).astype(BF16)

    def hidden_pair(hop):
        @pl.loop(0, 2)
        def _(d):
            hidden(lax.rem(z + jnp.where(d == 0, NZ - hop, hop), NZ))

    hidden(z)
    hidden_pair(1)
    forward(gu, 2)
    hidden_pair(2)
    forward(gu, 3)
    start(dn, 1)
    hidden_pair(3)
    arrive(gu)
    hidden(lax.rem(z + 4, NZ))

    def down(k, half):
        left = jnp.concatenate([units[half, o] for o in range(NZ)], axis=1)
        right = jnp.concatenate([dbuf[o, k * DC : (k + 1) * DC, :] for o in range(NZ)], axis=1)
        return lax.dot_general(left, right, (((1,), (1,)), ((), ())), preferred_element_type=F32)

    def partial_copy(k):
        return pltpu.make_async_remote_copy(
            src_ref=ps.at[k], dst_ref=pr.at[k], send_sem=ps_send.at[k], recv_sem=ps_recv.at[k],
            device_id=(ep, sib), device_id_type=MESH,
        )

    def back(k, peer, src):
        return pltpu.make_async_remote_copy(
            src_ref=rs.at[k, peer], dst_ref=rb.at[k, src],
            send_sem=rt_send.at[k, peer], recv_sem=rt_recv.at[k, src],
            device_id=(peer, tp), device_id_type=MESH,
        )

    def stage1(k):
        ps[k] = down(k, 1 - core).astype(BF16)
        partial_copy(k).start()
        acc[k] = down(k, core)

    def stage2(k):
        partial_copy(k).wait_recv()
        total = acc[k] + pr[k].astype(F32)
        rs[k] = total.reshape(NEP, CAP, DC).astype(BF16)

        @pl.loop(1, NEP)
        def _(j):
            back(k, lax.rem(ep + j, NEP), ep).start()

        rb[k, ep] = rs[k, ep]

    def stage3(k):
        @pl.loop(1, NEP)
        def _(j):
            src = lax.rem(ep + j, NEP)
            back(k, src, src).wait_recv()

        got = rb[k].astype(F32).reshape(ROWS, DC).astype(BF16)
        mixed = jnp.dot(comb[0], got, preferred_element_type=F32)
        mixed = mixed + jnp.dot(comb[1], got, preferred_element_type=F32)
        out_ref[:, k * DC : (k + 1) * DC] = mixed.astype(BF16)

    first, second = dn[:2], dn[2:]
    forward(first, 1)
    forward(first, 2)
    forward(first, 3)
    forward(second, 1)
    arrive(first)
    stage1(0)
    forward(second, 2)
    stage1(1)
    stage2(0)
    forward(second, 3)
    stage2(1)
    arrive(second[:1])
    stage1(2)
    arrive(second[1:])
    stage1(3)
    stage2(2)
    stage2(3)
    for k in range(NDC):
        stage3(k)

    for p in gu + dn:
        for d in (0, 1):
            for hop in (1, 2, 3, 4):
                ring(d, hop, p, sent(d, hop)).wait_send()

    @pl.loop(1, NEP)
    def _(k):
        peer = lax.rem(ep + k, NEP)
        dispatch(peer, ep).wait_send()
        for c in range(NDC):
            back(c, peer, ep).wait_send()

    to_sib.wait_send()
    for k in range(NDC):
        partial_copy(k).wait_send()


def expert_half(
    dispatched_group_activity,
    specialist_rmsgain,
    selected_specialist_ids,
    selected_specialist_share,
    specialist_switch_maps,
    specialist_widen_maps,
    specialist_shrink_maps,
):
    meta = jnp.concatenate(
        [selected_specialist_ids.astype(F32).T, selected_specialist_share.T, jnp.zeros((4, SHARD), F32)], axis=0
    )
    vm = pl.BlockSpec(memory_space=pltpu.VMEM)
    dma = pltpu.SemaphoreType.DMA
    return pl.pallas_call(
        expert_kernel,
        out_shape=jax.ShapeDtypeStruct((SHARD, DM), BF16),
        in_specs=[vm] * 6,
        out_specs=vm,
        scratch_shapes=[
            pltpu.VMEM((NZ, DM, SHARD), BF16),
            pltpu.VMEM((NZ, DM, SHARD), BF16),
            pltpu.VMEM((NZ, DM, SHARD), BF16),
            pltpu.VMEM((NEP, CAP, DM), BF16),
            pltpu.VMEM((2, NEP, CAP, DM), BF16),
            pltpu.VMEM((2, ROWS, DM), BF16),
            pltpu.VMEM((2, NZ, ROWS, SHARD), BF16),
            pltpu.VMEM((NDC, ROWS, DC), F32),
            pltpu.VMEM((NDC, ROWS, DC), BF16),
            pltpu.VMEM((NDC, ROWS, DC), BF16),
            pltpu.VMEM((NDC, NEP, CAP, DC), BF16),
            pltpu.VMEM((NDC, NEP, CAP, DC), BF16),
            pltpu.VMEM((2, SHARD, ROWS), BF16),
            dma((2, 4, NG + NDC)), dma((2, 4, NG + NDC)),
            dma((NEP,)), dma((NEP,)),
            dma, dma,
            dma((NDC,)), dma((NDC,)),
            dma((NDC, NEP)), dma((NDC, NEP)),
        ],
        compiler_params=pltpu.CompilerParams(
            collective_id=0, has_side_effects=True, vmem_limit_bytes=56 * 2**20
        ),
    )(
        dispatched_group_activity,
        specialist_rmsgain.reshape(1, DM),
        meta,
        specialist_switch_maps[0],
        specialist_widen_maps[0],
        specialist_shrink_maps[0],
    )


def on_device(
    scan_source_values,
    switch_path_values,
    causal_filter_coefficients,
    scan_switch_blockmap,
    entry_switch_blockmap,
    feature_fading_speeds,
    spike_amount,
    final_linear_map,
    dispatched_group_activity,
    specialist_rmsgain,
    selected_specialist_ids,
    selected_specialist_share,
    specialist_switch_maps,
    specialist_widen_maps,
    specialist_shrink_maps,
):
    scan_path_result = mixer_half(
        scan_source_values,
        switch_path_values,
        causal_filter_coefficients,
        scan_switch_blockmap,
        entry_switch_blockmap,
        feature_fading_speeds,
        spike_amount,
        final_linear_map,
    )
    moe_out = expert_half(
        dispatched_group_activity,
        specialist_rmsgain,
        selected_specialist_ids,
        selected_specialist_share,
        specialist_switch_maps,
        specialist_widen_maps,
        specialist_shrink_maps,
    )
    return (scan_path_result, moe_out)


def solution(mesh):
    in_specs = (
        P("tp", "ep"),
        P("tp", "ep"),
        P(),
        P(),
        P(),
        P(),
        P("ep"),
        P(),
        P(("ep", "tp"), None),
        P(),
        P(("ep", "tp"), None),
        P(("ep", "tp"), None),
        P("ep", None, "tp"),
        P("ep", None, "tp"),
        P("ep", None, "tp"),
    )
    out_specs = (P(("ep", "tp"), None), P(("ep", "tp"), None))
    return jax.shard_map(
        on_device, mesh=mesh, in_specs=in_specs, out_specs=out_specs, check_vma=False
    )
```

```python
import jax
import jax.numpy as jnp
from jax import lax
from jax.experimental import pallas as pl
from jax.experimental.pallas import tpu as pltpu
from jax.sharding import PartitionSpec as P

MESH = pl.DeviceIdType.MESH
F32 = jnp.float32
BF16 = jnp.bfloat16
CAP = 24
ROWS = 384
DM = 2048
SHARD = 128
NZ = 8
NEP = 16
NDC = 8
DC = DM // NDC
NG = 4
GROWS = 1024
POS = 2048
HALO = 128
SPAN = 512
CH = 64


def whole_kernel(
    gain_hbm, id_hbm, share_hbm, taps_hbm, rate_hbm, entry_hbm, fading_hbm, spike_hbm,
    src_hbm, gate_hbm, map_hbm, tok_hbm, g_hbm, u_hbm, d_hbm, scan_ref, out_ref,
    gbuf, ubuf, dbuf, snd, xin, xmat, units, acc, ps, pr, rs, rb, comb,
    gain_ref, id_ref, share_ref, taps_ref, rate_ref, entry_ref, fading_ref, spike_ref,
    tok_ref, src_ref, gate_ref, map_ref, state_buf, decay_buf, tot_out, tot_in, mix_out, mix_in,
    ag_send, ag_recv, ds_send, ds_recv, xs_send, xs_recv, ps_send, ps_recv, rt_send, rt_recv,
    scan_out, out_buf, in_sem, out_sem, halo_send, halo_recv, tt_send, tt_recv, mx_send, mx_recv,
):
    ep = lax.axis_index("ep")
    tp = lax.axis_index("tp")
    z = tp // 2
    core = lax.rem(tp, 2)
    sib = z * 2 + (1 - core)
    nbr = (lax.rem(z + 1, NZ) * 2 + core, lax.rem(z + NZ - 1, NZ) * 2 + core)

    loads = [
        pltpu.make_async_copy(src, dst, in_sem.at[i])
        for i, (src, dst) in enumerate(
            (
                (g_hbm, gbuf.at[z]),
                (u_hbm, ubuf.at[z]),
                (tok_hbm, tok_ref),
                (src_hbm, src_ref.at[:, pl.ds(HALO, POS)]),
                (d_hbm, dbuf.at[z]),
                (gate_hbm, gate_ref),
                (map_hbm, map_ref),
                (gain_hbm, gain_ref),
                (id_hbm, id_ref),
                (share_hbm, share_ref),
                (taps_hbm, taps_ref),
                (rate_hbm.at[tp], rate_ref),
                (entry_hbm.at[tp], entry_ref),
                (fading_hbm, fading_ref),
                (spike_hbm, spike_ref),
            )
        )
    ]
    for load in loads:
        load.start()

    bar = pltpu.get_barrier_semaphore()

    @pl.loop(1, NEP)
    def _(k):
        pl.semaphore_signal(bar, inc=1, device_id=(lax.rem(ep + k, NEP), tp), device_id_type=MESH)
        pl.semaphore_signal(bar, inc=1, device_id=(ep, lax.rem(tp + k, NEP)), device_id_type=MESH)

    pl.semaphore_wait(bar, 2 * (NEP - 1))

    def piece(p):
        if p < NG:
            return (gbuf if p < 2 else ubuf, (p % 2) * GROWS, GROWS)
        return dbuf, (p - NG) * DC, DC

    def ring(d, hop, p, origin):
        buf, lo, n = piece(p)
        last = isinstance(hop, int) and hop == 4
        if last:
            n = n // 2
            lo = lo + d * n
        return pltpu.make_async_remote_copy(
            src_ref=buf.at[origin, pl.ds(lo, n)], dst_ref=buf.at[origin, pl.ds(lo, n)],
            send_sem=ag_send.at[d, hop - 1, p], recv_sem=ag_recv.at[d, hop - 1, p],
            device_id=(ep, nbr[d]), device_id_type=MESH,
        )

    def sent(d, hop):
        return lax.rem(z + NZ - (hop - 1), NZ) if d == 0 else lax.rem(z + hop - 1, NZ)

    def came(d, hop):
        return lax.rem(z + NZ - hop, NZ) if d == 0 else lax.rem(z + hop, NZ)

    def start(pieces, hop):
        for p in pieces:
            for d in (0, 1):
                ring(d, hop, p, sent(d, hop)).start()

    def forward(pieces, hop, last=False):
        for p in pieces:
            for d in (0, 1):
                ring(d, hop, p, came(d, hop)).wait_recv()
                nxt = 4 if last else hop + 1
                ring(d, nxt, p, sent(d, nxt)).start()

    def arrive(pieces):
        for p in pieces:
            for d in (0, 1):
                ring(d, 4, p, came(d, 4)).wait_recv()

    gu = list(range(NG))
    dn = list(range(NG, NG + NDC))
    loads[0].wait()
    loads[1].wait()
    start(gu, 1)
    for i in (2, 3, 7, 8, 9, 10, 11, 12, 13, 14):
        loads[i].wait()
    halo = pltpu.make_async_remote_copy(
        src_ref=src_ref.at[:, pl.ds(POS, HALO)], dst_ref=src_ref.at[:, pl.ds(0, HALO)],
        send_sem=halo_send, recv_sem=halo_recv,
        device_id=(lax.rem(ep + 1, NEP), tp), device_id_type=MESH,
    )
    halo.start()

    values = tok_ref[...].astype(F32)
    scale = lax.rsqrt(jnp.mean(values * values, axis=1, keepdims=True) + 1e-06)
    gains = gain_ref[...].astype(F32)
    gain = jnp.concatenate([gains[i : i + 1, :] for i in range(NEP)], axis=1)
    normed = (values * scale * gain).astype(BF16)
    expert_no = lax.broadcasted_iota(jnp.int32, (NEP, SHARD), 0).astype(F32)
    ids = id_ref[...].astype(F32)
    is0 = ids[0:1, :] == expert_no
    is1 = ids[1:2, :] == expert_no
    member = jnp.where(is0 | is1, 1.0, 0.0)
    weight = jnp.where(is0, share_ref[0:1, :], 0.0) + jnp.where(is1, share_ref[1:2, :], 0.0)
    before = (
        lax.broadcasted_iota(jnp.int32, (SHARD, SHARD), 0)
        < lax.broadcasted_iota(jnp.int32, (SHARD, SHARD), 1)
    )
    rank = jnp.dot(
        member.astype(BF16), jnp.where(before, 1.0, 0.0).astype(BF16), preferred_element_type=F32
    )
    place = jnp.where(member > 0.0, rank, -1.0)
    slot_no = lax.broadcasted_iota(jnp.int32, (CAP, SHARD), 0).astype(F32)
    picks, shares = [], []
    for e in range(NEP):
        hit = place[e : e + 1, :] == slot_no
        picks.append(jnp.where(hit, 1.0, 0.0))
        shares.append(jnp.where(hit, weight[e : e + 1, :], 0.0))
    pick = jnp.concatenate(picks, axis=0).astype(BF16)
    share = jnp.concatenate(shares, axis=0).T
    share_hi = share.astype(BF16)
    comb[0] = share_hi
    comb[1] = (share - share_hi.astype(F32)).astype(BF16)
    for k in range(4):
        rows = jnp.dot(pick, normed[:, k * 512 : (k + 1) * 512], preferred_element_type=F32)
        snd[:, :, k * 512 : (k + 1) * 512] = rows.reshape(NEP, CAP, 512).astype(BF16)

    def dispatch(peer, src):
        return pltpu.make_async_remote_copy(
            src_ref=snd.at[peer], dst_ref=xin.at[core, src],
            send_sem=ds_send.at[peer], recv_sem=ds_recv.at[src],
            device_id=(peer, tp), device_id_type=MESH,
        )

    @pl.loop(1, NEP)
    def _(k):
        dispatch(lax.rem(ep + k, NEP), ep).start()

    xin[core, ep] = snd[ep]

    lanes = pl.ds(pl.multiple_of(z * SHARD, SHARD), SHARD)
    taps = jnp.concatenate([taps_ref[:, lanes].astype(F32), jnp.zeros((4, SHARD), F32)], axis=0)
    taps = jnp.concatenate([taps] * 16, axis=0).T
    taps = jnp.where(core == 0, taps[:CH], taps[CH:])
    gates = jnp.concatenate([rate_ref[...].astype(F32).T, entry_ref[...].astype(F32).T], axis=0).astype(BF16)
    speeds = jnp.broadcast_to(fading_ref[pl.ds(z, 1), :], (SHARD, SHARD)).T
    speed = jnp.where(core == 0, speeds[:CH, 0:1], speeds[CH:, 0:1]) * -8.0
    halo.wait_recv()
    place_no = lax.broadcasted_iota(jnp.int32, (CH, SPAN), 1)
    back_no = lax.broadcasted_iota(jnp.int32, (CH, SPAN + HALO), 1)

    def local(k, carry):
        at = pl.multiple_of(k * SPAN, SPAN)
        span = src_ref[:, pl.ds(at, SPAN + HALO)].astype(F32)
        span = jnp.where((back_no < HALO) & (k == 0) & (ep == 0), 0.0, span)
        running = pltpu.roll(span, 3, 1)[:, HALO:] * taps[:, 0:1]
        running = running + pltpu.roll(span, 2, 1)[:, HALO:] * taps[:, 1:2]
        running = running + pltpu.roll(span, 1, 1)[:, HALO:] * taps[:, 2:3]
        running = running + span[:, HALO:] * taps[:, 3:4]
        conv = running.astype(BF16)
        both = jax.nn.sigmoid(jnp.dot(gates, conv, preferred_element_type=F32))
        power = both[:CH] * speed + spike_ref[:, pl.ds(at, SPAN)]
        decay = jnp.exp(power)
        twice = 2.0 * power
        series = 1.0 + twice * (1.0 / 7.0)
        for n in (6.0, 5.0, 4.0, 3.0, 2.0):
            series = 1.0 + twice * (1.0 / n) * series
        left = jnp.where(twice > -0.25, -twice * series, 1.0 - decay * decay)
        drive = jnp.sqrt(left) * both[CH:] * conv.astype(F32)
        step = 1
        while step < SPAN:
            inside = place_no >= step
            drive = drive + decay * jnp.where(inside, pltpu.roll(drive, step, 1), 0.0)
            decay = decay * jnp.where(inside, pltpu.roll(decay, step, 1), 1.0)
            step *= 2
        drive = drive + decay * carry[1]
        decay = decay * carry[0]
        state_buf[:, pl.ds(at, SPAN)] = drive
        decay_buf[:, pl.ds(at, SPAN)] = decay
        return decay[:, SPAN - 1 :], drive[:, SPAN - 1 :]

    ends = lax.fori_loop(0, POS // SPAN, local, (jnp.ones((CH, 1), F32), jnp.zeros((CH, 1), F32)))
    lane = lax.broadcasted_iota(jnp.int32, (CH, SHARD), 1)
    packed = jnp.where(lane == 0, ends[0], jnp.where(lane == 1, ends[1], 0.0))
    tot_out[...] = jnp.concatenate([packed, jnp.zeros((CH, SHARD), F32)], axis=0).T[0:8, :]

    def total(peer, src):
        return pltpu.make_async_remote_copy(
            src_ref=tot_out, dst_ref=tot_in.at[src], send_sem=tt_send.at[peer], recv_sem=tt_recv.at[src],
            device_id=(peer, tp), device_id_type=MESH,
        )

    @pl.loop(1, NEP)
    def _(k):
        total(lax.rem(ep + k, NEP), ep).start()

    tot_in[ep] = tot_out[...]
    forward(gu, 1)

    @pl.loop(1, NEP)
    def _(k):
        src = lax.rem(ep + k, NEP)
        total(src, src).wait_recv()

    entering = jnp.zeros((1, SHARD), F32)
    for src in range(NEP - 1):
        earlier = src < ep
        entering = jnp.where(earlier, tot_in[src, 0:1, :] * entering + tot_in[src, 1:2, :], entering)
    entering = jnp.broadcast_to(entering, (SHARD, SHARD)).T[:CH, 0:1]
    loads[5].wait()

    @pl.loop(0, POS // SPAN)
    def _(k):
        at = pl.multiple_of(k * SPAN, SPAN)
        state = state_buf[:, pl.ds(at, SPAN)] + decay_buf[:, pl.ds(at, SPAN)] * entering
        side = gate_ref[:, pl.ds(at, SPAN)].astype(F32)
        mixed = (state * jax.nn.gelu(side, approximate=True)).astype(BF16)
        for i in range(SPAN // SHARD):
            mix_out[k * (SPAN // SHARD) + i] = mixed[:, i * SHARD : (i + 1) * SHARD]

    def hand(peer, src):
        return pltpu.make_async_remote_copy(
            src_ref=mix_out.at[peer], dst_ref=mix_in.at[src], send_sem=mx_send.at[peer], recv_sem=mx_recv.at[src],
            device_id=(ep, peer), device_id_type=MESH,
        )

    mix_in[tp] = mix_out[tp]

    @pl.loop(1, NEP)
    def _(k):
        src = lax.rem(ep + k, NEP)
        dispatch(src, src).wait_recv()

    to_sib = pltpu.make_async_remote_copy(
        src_ref=xin.at[core], dst_ref=xin.at[core], send_sem=xs_send, recv_sem=xs_recv,
        device_id=(ep, sib), device_id_type=MESH,
    )
    from_sib = pltpu.make_async_remote_copy(
        src_ref=xin.at[1 - core], dst_ref=xin.at[1 - core], send_sem=xs_send, recv_sem=xs_recv,
        device_id=(ep, sib), device_id_type=MESH,
    )
    to_sib.start()
    from_sib.wait_recv()

    @pl.loop(0, 2 * (NEP // 2))
    def _(i):
        half = i // (NEP // 2)
        pair = lax.rem(i, NEP // 2)
        two = xin[half, pl.ds(pair * 2, 2)].astype(F32).reshape(2 * CAP, DM)
        xmat[half, pl.ds(pl.multiple_of(pair * 2 * CAP, 16), 2 * CAP), :] = two.astype(BF16)

    def hidden(origin):
        @pl.loop(0, 2)
        def _(half):
            both = jnp.concatenate([gbuf[origin], ubuf[origin]], axis=1)
            pre = jnp.dot(xmat[half], both, preferred_element_type=F32)
            gate = jnp.minimum(pre[:, :SHARD], 7.0)
            up = jnp.clip(pre[:, SHARD:], -7.0, 7.0)
            units[half, origin] = ((up + 1.0) * gate * jax.nn.sigmoid(1.702 * gate)).astype(BF16)

    def hidden_pair(hop):
        @pl.loop(0, 2)
        def _(d):
            hidden(lax.rem(z + jnp.where(d == 0, NZ - hop, hop), NZ))

    hidden(z)
    hidden_pair(1)
    forward(gu, 2)
    hidden_pair(2)
    forward(gu, 3)
    loads[4].wait()
    start(dn, 1)
    hidden_pair(3)

    arrive(gu)
    hidden(lax.rem(z + 4, NZ))

    def down(k, half):
        left = jnp.concatenate([units[half, o] for o in range(NZ)], axis=1)
        right = jnp.concatenate([dbuf[o, k * DC : (k + 1) * DC, :] for o in range(NZ)], axis=1)
        return lax.dot_general(left, right, (((1,), (1,)), ((), ())), preferred_element_type=F32)

    def partial_copy(k):
        return pltpu.make_async_remote_copy(
            src_ref=ps.at[k], dst_ref=pr.at[k], send_sem=ps_send.at[k], recv_sem=ps_recv.at[k],
            device_id=(ep, sib), device_id_type=MESH,
        )

    def back(k, peer, src):
        return pltpu.make_async_remote_copy(
            src_ref=rs.at[k, peer], dst_ref=rb.at[k, src],
            send_sem=rt_send.at[k, peer], recv_sem=rt_recv.at[k, src],
            device_id=(peer, tp), device_id_type=MESH,
        )

    def stage1(k):
        ps[k] = down(k, 1 - core).astype(BF16)
        partial_copy(k).start()
        acc[k] = down(k, core)

    def stage2(k):
        partial_copy(k).wait_recv()
        total = acc[k] + pr[k].astype(F32)
        rs[k] = total.reshape(NEP, CAP, DC).astype(BF16)

        @pl.loop(1, NEP)
        def _(j):
            back(k, lax.rem(ep + j, NEP), ep).start()

        rb[k, ep] = rs[k, ep]

    def out_copy(k):
        cols = pl.ds(k * DC, DC)
        return pltpu.make_async_copy(out_buf.at[:, cols], out_ref.at[:, cols], out_sem.at[k])

    def stage3(k):
        @pl.loop(1, NEP)
        def _(j):
            src = lax.rem(ep + j, NEP)
            back(k, src, src).wait_recv()

        got = rb[k].astype(F32).reshape(ROWS, DC).astype(BF16)
        mixed = jnp.dot(comb[0], got, preferred_element_type=F32)
        mixed = mixed + jnp.dot(comb[1], got, preferred_element_type=F32)
        out_buf[:, k * DC : (k + 1) * DC] = mixed.astype(BF16)
        out_copy(k).start()

    for i in range(NDC + 6):
        if i < NDC:
            forward(dn[i : i + 1], 1)
        if 0 <= i - 1 < NDC:
            forward(dn[i - 1 : i], 2)
        if 0 <= i - 2 < NDC:
            forward(dn[i - 2 : i - 1], 3)
        if i - 2 == NDC - 1:
            @pl.loop(1, NEP)
            def _(k):
                hand(lax.rem(tp + k, NEP), tp).start()

        if 0 <= i - 4 < NDC:
            stage2(i - 4)
        if 0 <= i - 3 < NDC:
            arrive(dn[i - 3 : i - 2])
            stage1(i - 3)
        if 0 <= i - 6 < NDC - 1:
            stage3(i - 6)
        if i - 6 == NDC - 2:
            loads[6].wait()

            @pl.loop(1, NEP)
            def _(k):
                src = lax.rem(tp + k, NEP)
                hand(src, src).wait_recv()

            hidden_rows = mix_in[...].reshape(NEP * CH, SHARD).astype(F32).T.astype(BF16)

            @pl.loop(0, 4)
            def _(k):
                cols = pl.ds(pl.multiple_of(k * 512, 512), 512)
                scan_out[:, cols] = jnp.dot(hidden_rows, map_ref[:, cols], preferred_element_type=F32).astype(BF16)

            scan_copy = pltpu.make_async_copy(scan_out, scan_ref, out_sem.at[NDC])
            scan_copy.start()
        if i - 6 == NDC - 1:
            stage3(NDC - 1)

    for p in gu + dn:
        for d in (0, 1):
            for hop in (1, 2, 3, 4):
                ring(d, hop, p, sent(d, hop)).wait_send()

    @pl.loop(1, NEP)
    def _(k):
        peer = lax.rem(ep + k, NEP)
        dispatch(peer, ep).wait_send()
        for c in range(NDC):
            back(c, peer, ep).wait_send()

    @pl.loop(1, NEP)
    def _(k):
        total(lax.rem(ep + k, NEP), ep).wait_send()
        hand(lax.rem(tp + k, NEP), tp).wait_send()

    scan_copy.wait()
    for k in range(NDC):
        out_copy(k).wait()
    halo.wait_send()
    to_sib.wait_send()
    for k in range(NDC):
        partial_copy(k).wait_send()


def on_device(
    scan_source_values,
    switch_path_values,
    causal_filter_coefficients,
    scan_switch_blockmap,
    entry_switch_blockmap,
    feature_fading_speeds,
    spike_amount,
    final_linear_map,
    dispatched_group_activity,
    specialist_rmsgain,
    selected_specialist_ids,
    selected_specialist_share,
    specialist_switch_maps,
    specialist_widen_maps,
    specialist_shrink_maps,
):
    hbm = pl.BlockSpec(memory_space=pltpu.HBM)
    dma = pltpu.SemaphoreType.DMA
    result = jax.ShapeDtypeStruct((SHARD, DM), BF16)
    computed = pl.pallas_call(
        whole_kernel,
        out_shape=(result, result),
        in_specs=[hbm] * 15,
        out_specs=(hbm, hbm),
        scratch_shapes=[
            pltpu.VMEM((NZ, DM, SHARD), BF16),
            pltpu.VMEM((NZ, DM, SHARD), BF16),
            pltpu.VMEM((NZ, DM, SHARD), BF16),
            pltpu.VMEM((NEP, CAP, DM), BF16),
            pltpu.VMEM((2, NEP, CAP, DM), BF16),
            pltpu.VMEM((2, ROWS, DM), BF16),
            pltpu.VMEM((2, NZ, ROWS, SHARD), BF16),
            pltpu.VMEM((NDC, ROWS, DC), F32),
            pltpu.VMEM((NDC, ROWS, DC), BF16),
            pltpu.VMEM((NDC, ROWS, DC), BF16),
            pltpu.VMEM((NDC, NEP, CAP, DC), BF16),
            pltpu.VMEM((NDC, NEP, CAP, DC), BF16),
            pltpu.VMEM((2, SHARD, ROWS), BF16),
            pltpu.VMEM((NEP, SHARD), BF16),
            pltpu.VMEM((2, SHARD), jnp.int32),
            pltpu.VMEM((2, SHARD), F32),
            pltpu.VMEM((4, NZ * SHARD), BF16),
            pltpu.VMEM((CH, CH), BF16),
            pltpu.VMEM((CH, CH), BF16),
            pltpu.VMEM((NZ, SHARD), F32),
            pltpu.VMEM((1, POS), F32),
            pltpu.VMEM((SHARD, DM), BF16),
            pltpu.VMEM((CH, HALO + POS), BF16),
            pltpu.VMEM((CH, POS), BF16),
            pltpu.VMEM((NEP * CH, DM), BF16),
            pltpu.VMEM((CH, POS), F32),
            pltpu.VMEM((CH, POS), F32),
            pltpu.VMEM((8, SHARD), F32),
            pltpu.VMEM((NEP, 8, SHARD), F32),
            pltpu.VMEM((NEP, CH, SHARD), BF16),
            pltpu.VMEM((NEP, CH, SHARD), BF16),
            dma((2, 4, NG + NDC)), dma((2, 4, NG + NDC)),
            dma((NEP,)), dma((NEP,)),
            dma, dma,
            dma((NDC,)), dma((NDC,)),
            dma((NDC, NEP)), dma((NDC, NEP)),
            pltpu.VMEM((SHARD, DM), BF16),
            pltpu.VMEM((SHARD, DM), BF16),
            dma((15,)), dma((NDC + 1,)), dma, dma,
            dma((NEP,)), dma((NEP,)),
            dma((NEP,)), dma((NEP,)),
        ],
        compiler_params=pltpu.CompilerParams(
            collective_id=0, has_side_effects=True, vmem_limit_bytes=62 * 2**20
        ),
    )(
        specialist_rmsgain.reshape(NEP, SHARD),
        selected_specialist_ids.T,
        selected_specialist_share.T,
        causal_filter_coefficients.T,
        scan_switch_blockmap,
        entry_switch_blockmap,
        feature_fading_speeds.reshape(8, SHARD),
        spike_amount.reshape(1, POS),
        scan_source_values,
        switch_path_values,
        final_linear_map,
        dispatched_group_activity,
        specialist_switch_maps[0],
        specialist_widen_maps[0],
        specialist_shrink_maps[0],
    )
    return pl.pallas_call(
        handover_kernel,
        out_shape=(result, result),
        in_specs=[hbm] * 2,
        out_specs=(hbm, hbm),
        scratch_shapes=[pltpu.VMEM((4, SHARD // 2, DM), BF16), dma((4,)), dma((4,))],
    )(*computed)


def handover_kernel(scan_in, moe_in, scan_ref, moe_ref, stage, in_sem, out_sem):
    half = SHARD // 2
    parts = [(a, b, pl.ds(h * half, half)) for a, b in ((scan_in, scan_ref), (moe_in, moe_ref)) for h in (0, 1)]
    ins = [pltpu.make_async_copy(a.at[r], stage.at[i], in_sem.at[i]) for i, (a, b, r) in enumerate(parts)]
    outs = [pltpu.make_async_copy(stage.at[i], b.at[r], out_sem.at[i]) for i, (a, b, r) in enumerate(parts)]
    for copy in ins:
        copy.start()
    for i in range(4):
        ins[i].wait()
        outs[i].start()
    for copy in outs:
        copy.wait()


def solution(mesh):
    in_specs = (
        P("tp", "ep"),
        P("tp", "ep"),
        P(),
        P(),
        P(),
        P(),
        P("ep"),
        P(),
        P(("ep", "tp"), None),
        P(),
        P(("ep", "tp"), None),
        P(("ep", "tp"), None),
        P("ep", None, "tp"),
        P("ep", None, "tp"),
        P("ep", None, "tp"),
    )
    out_specs = (P(("ep", "tp"), None), P(("ep", "tp"), None))
    return jax.shard_map(
        on_device, mesh=mesh, in_specs=in_specs, out_specs=out_specs, check_vma=False
    )
```

```python
import jax
import jax.numpy as jnp
from jax import lax
from jax.experimental import pallas as pl
from jax.experimental.pallas import tpu as pltpu
from jax.sharding import PartitionSpec as P

MESH = pl.DeviceIdType.MESH
F32 = jnp.float32
BF16 = jnp.bfloat16
CAP = 24
ROWS = 384
DM = 2048
SHARD = 128
NZ = 8
NEP = 16
DCS = (512, 512, 256, 256, 256, 256)
NDC = len(DCS)
NG = 4
GROWS = 1024
POS = 2048
HALO = 128
SPAN = 512
CH = 64


def whole_kernel(
    gain_hbm, id_hbm, share_hbm, taps_hbm, rate_hbm, entry_hbm, fading_hbm, spike_hbm,
    src_hbm, gate_hbm, map_hbm, tok_hbm, g_hbm, u_hbm, d_hbm, scan_ref, out_ref,
    gbuf, ubuf, dbuf, snd, xin, xmat, units, acc, ps, pr, rs, rb, comb,
    gain_ref, id_ref, share_ref, taps_ref, rate_ref, entry_ref, fading_ref, spike_ref,
    tok_ref, src_ref, gate_ref, map_ref, state_buf, decay_buf, tot_out, tot_in, mix_out, mix_in,
    ag_send, ag_recv, ds_send, ds_recv, xs_send, xs_recv, ps_send, ps_recv, rt_send, rt_recv,
    scan_out, out_buf, in_sem, out_sem, halo_send, halo_recv, tt_send, tt_recv, mx_send, mx_recv,
):
    ep = lax.axis_index("ep")
    tp = lax.axis_index("tp")
    z = tp // 2
    core = lax.rem(tp, 2)
    sib = z * 2 + (1 - core)
    nbr = (lax.rem(z + 1, NZ) * 2 + core, lax.rem(z + NZ - 1, NZ) * 2 + core)

    loads = [
        pltpu.make_async_copy(src, dst, in_sem.at[i])
        for i, (src, dst) in enumerate(
            (
                (g_hbm, gbuf.at[z]),
                (u_hbm, ubuf.at[z]),
                (tok_hbm, tok_ref),
                (src_hbm, src_ref.at[:, pl.ds(HALO, POS)]),
                (d_hbm, dbuf.at[z]),
                (gate_hbm, gate_ref),
                (map_hbm, map_ref),
                (gain_hbm, gain_ref),
                (id_hbm, id_ref),
                (share_hbm, share_ref),
                (taps_hbm, taps_ref),
                (rate_hbm.at[tp], rate_ref),
                (entry_hbm.at[tp], entry_ref),
                (fading_hbm, fading_ref),
                (spike_hbm, spike_ref),
            )
        )
    ]
    for load in loads:
        load.start()

    bar = pltpu.get_barrier_semaphore()

    @pl.loop(1, NEP)
    def _(k):
        pl.semaphore_signal(bar, inc=1, device_id=(lax.rem(ep + k, NEP), tp), device_id_type=MESH)
        pl.semaphore_signal(bar, inc=1, device_id=(ep, lax.rem(tp + k, NEP)), device_id_type=MESH)

    pl.semaphore_wait(bar, 2 * (NEP - 1))

    def piece(p):
        if p < NG:
            return (gbuf if p < 2 else ubuf, (p % 2) * GROWS, GROWS)
        return dbuf, sum(DCS[: p - NG]), DCS[p - NG]

    def ring(d, hop, p, origin):
        buf, lo, n = piece(p)
        last = isinstance(hop, int) and hop == 4
        if last:
            n = n // 2
            lo = lo + d * n
        return pltpu.make_async_remote_copy(
            src_ref=buf.at[origin, pl.ds(lo, n)], dst_ref=buf.at[origin, pl.ds(lo, n)],
            send_sem=ag_send.at[d, hop - 1, p], recv_sem=ag_recv.at[d, hop - 1, p],
            device_id=(ep, nbr[d]), device_id_type=MESH,
        )

    def sent(d, hop):
        return lax.rem(z + NZ - (hop - 1), NZ) if d == 0 else lax.rem(z + hop - 1, NZ)

    def came(d, hop):
        return lax.rem(z + NZ - hop, NZ) if d == 0 else lax.rem(z + hop, NZ)

    def start(pieces, hop):
        for p in pieces:
            for d in (0, 1):
                ring(d, hop, p, sent(d, hop)).start()

    def forward(pieces, hop, last=False):
        for p in pieces:
            for d in (0, 1):
                ring(d, hop, p, came(d, hop)).wait_recv()
                nxt = 4 if last else hop + 1
                ring(d, nxt, p, sent(d, nxt)).start()

    def arrive(pieces):
        for p in pieces:
            for d in (0, 1):
                ring(d, 4, p, came(d, 4)).wait_recv()

    gu = list(range(NG))
    dn = list(range(NG, NG + NDC))
    loads[0].wait()
    loads[1].wait()
    start(gu, 1)
    for i in (2, 3, 7, 8, 9, 10, 11, 12, 13, 14):
        loads[i].wait()
    halo = pltpu.make_async_remote_copy(
        src_ref=src_ref.at[:, pl.ds(POS, HALO)], dst_ref=src_ref.at[:, pl.ds(0, HALO)],
        send_sem=halo_send, recv_sem=halo_recv,
        device_id=(lax.rem(ep + 1, NEP), tp), device_id_type=MESH,
    )
    halo.start()

    values = tok_ref[...].astype(F32)
    scale = lax.rsqrt(jnp.mean(values * values, axis=1, keepdims=True) + 1e-06)
    gains = gain_ref[...].astype(F32)
    gain = jnp.concatenate([gains[i : i + 1, :] for i in range(NEP)], axis=1)
    normed = (values * scale * gain).astype(BF16)
    expert_no = lax.broadcasted_iota(jnp.int32, (NEP, SHARD), 0).astype(F32)
    ids = id_ref[...].astype(F32)
    is0 = ids[0:1, :] == expert_no
    is1 = ids[1:2, :] == expert_no
    member = jnp.where(is0 | is1, 1.0, 0.0)
    weight = jnp.where(is0, share_ref[0:1, :], 0.0) + jnp.where(is1, share_ref[1:2, :], 0.0)
    before = (
        lax.broadcasted_iota(jnp.int32, (SHARD, SHARD), 0)
        < lax.broadcasted_iota(jnp.int32, (SHARD, SHARD), 1)
    )
    rank = jnp.dot(
        member.astype(BF16), jnp.where(before, 1.0, 0.0).astype(BF16), preferred_element_type=F32
    )
    place = jnp.where(member > 0.0, rank, -1.0)
    slot_no = lax.broadcasted_iota(jnp.int32, (CAP, SHARD), 0).astype(F32)
    picks, shares = [], []
    for e in range(NEP):
        hit = place[e : e + 1, :] == slot_no
        picks.append(jnp.where(hit, 1.0, 0.0))
        shares.append(jnp.where(hit, weight[e : e + 1, :], 0.0))
    pick = jnp.concatenate(picks, axis=0).astype(BF16)
    share = jnp.concatenate(shares, axis=0).T
    share_hi = share.astype(BF16)
    comb[0] = share_hi
    comb[1] = (share - share_hi.astype(F32)).astype(BF16)
    for k in range(4):
        rows = jnp.dot(pick, normed[:, k * 512 : (k + 1) * 512], preferred_element_type=F32)
        snd[:, :, k * 512 : (k + 1) * 512] = rows.reshape(NEP, CAP, 512).astype(BF16)

    def dispatch(peer, src):
        return pltpu.make_async_remote_copy(
            src_ref=snd.at[peer], dst_ref=xin.at[core, src],
            send_sem=ds_send.at[peer], recv_sem=ds_recv.at[src],
            device_id=(peer, tp), device_id_type=MESH,
        )

    @pl.loop(1, NEP)
    def _(k):
        dispatch(lax.rem(ep + k, NEP), ep).start()

    xin[core, ep] = snd[ep]

    lanes = pl.ds(pl.multiple_of(z * SHARD, SHARD), SHARD)
    taps = jnp.concatenate([taps_ref[:, lanes].astype(F32), jnp.zeros((4, SHARD), F32)], axis=0)
    taps = jnp.concatenate([taps] * 16, axis=0).T
    taps = jnp.where(core == 0, taps[:CH], taps[CH:])
    gates = jnp.concatenate([rate_ref[...].astype(F32).T, entry_ref[...].astype(F32).T], axis=0).astype(BF16)
    speeds = jnp.broadcast_to(fading_ref[pl.ds(z, 1), :], (SHARD, SHARD)).T
    speed = jnp.where(core == 0, speeds[:CH, 0:1], speeds[CH:, 0:1]) * -8.0
    halo.wait_recv()
    place_no = lax.broadcasted_iota(jnp.int32, (CH, SPAN), 1)
    back_no = lax.broadcasted_iota(jnp.int32, (CH, SPAN + HALO), 1)

    def local(k, carry):
        at = pl.multiple_of(k * SPAN, SPAN)
        span = src_ref[:, pl.ds(at, SPAN + HALO)].astype(F32)
        span = jnp.where((back_no < HALO) & (k == 0) & (ep == 0), 0.0, span)
        running = pltpu.roll(span, 3, 1)[:, HALO:] * taps[:, 0:1]
        running = running + pltpu.roll(span, 2, 1)[:, HALO:] * taps[:, 1:2]
        running = running + pltpu.roll(span, 1, 1)[:, HALO:] * taps[:, 2:3]
        running = running + span[:, HALO:] * taps[:, 3:4]
        conv = running.astype(BF16)
        both = jax.nn.sigmoid(jnp.dot(gates, conv, preferred_element_type=F32))
        power = both[:CH] * speed + spike_ref[:, pl.ds(at, SPAN)]
        decay = jnp.exp(power)
        twice = 2.0 * power
        series = 1.0 + twice * (1.0 / 7.0)
        for n in (6.0, 5.0, 4.0, 3.0, 2.0):
            series = 1.0 + twice * (1.0 / n) * series
        left = jnp.where(twice > -0.25, -twice * series, 1.0 - decay * decay)
        drive = jnp.sqrt(left) * both[CH:] * conv.astype(F32)
        step = 1
        while step < SPAN:
            inside = place_no >= step
            drive = drive + decay * jnp.where(inside, pltpu.roll(drive, step, 1), 0.0)
            decay = decay * jnp.where(inside, pltpu.roll(decay, step, 1), 1.0)
            step *= 2
        drive = drive + decay * carry[1]
        decay = decay * carry[0]
        state_buf[:, pl.ds(at, SPAN)] = drive
        decay_buf[:, pl.ds(at, SPAN)] = decay
        return decay[:, SPAN - 1 :], drive[:, SPAN - 1 :]

    ends = lax.fori_loop(0, POS // SPAN, local, (jnp.ones((CH, 1), F32), jnp.zeros((CH, 1), F32)))
    lane = lax.broadcasted_iota(jnp.int32, (CH, SHARD), 1)
    packed = jnp.where(lane == 0, ends[0], jnp.where(lane == 1, ends[1], 0.0))
    tot_out[...] = jnp.concatenate([packed, jnp.zeros((CH, SHARD), F32)], axis=0).T[0:8, :]

    def total(peer, src):
        return pltpu.make_async_remote_copy(
            src_ref=tot_out, dst_ref=tot_in.at[src], send_sem=tt_send.at[peer], recv_sem=tt_recv.at[src],
            device_id=(peer, tp), device_id_type=MESH,
        )

    @pl.loop(1, NEP)
    def _(k):
        total(lax.rem(ep + k, NEP), ep).start()

    tot_in[ep] = tot_out[...]
    forward(gu, 1)

    @pl.loop(1, NEP)
    def _(k):
        src = lax.rem(ep + k, NEP)
        total(src, src).wait_recv()

    entering = jnp.zeros((1, SHARD), F32)
    for src in range(NEP - 1):
        earlier = src < ep
        entering = jnp.where(earlier, tot_in[src, 0:1, :] * entering + tot_in[src, 1:2, :], entering)
    entering = jnp.broadcast_to(entering, (SHARD, SHARD)).T[:CH, 0:1]
    loads[5].wait()

    @pl.loop(0, POS // SPAN)
    def _(k):
        at = pl.multiple_of(k * SPAN, SPAN)
        state = state_buf[:, pl.ds(at, SPAN)] + decay_buf[:, pl.ds(at, SPAN)] * entering
        side = gate_ref[:, pl.ds(at, SPAN)].astype(F32)
        mixed = (state * jax.nn.gelu(side, approximate=True)).astype(BF16)
        for i in range(SPAN // SHARD):
            mix_out[k * (SPAN // SHARD) + i] = mixed[:, i * SHARD : (i + 1) * SHARD]

    def hand(peer, src):
        return pltpu.make_async_remote_copy(
            src_ref=mix_out.at[peer], dst_ref=mix_in.at[src], send_sem=mx_send.at[peer], recv_sem=mx_recv.at[src],
            device_id=(ep, peer), device_id_type=MESH,
        )

    mix_in[tp] = mix_out[tp]

    @pl.loop(1, NEP)
    def _(k):
        src = lax.rem(ep + k, NEP)
        dispatch(src, src).wait_recv()

    to_sib = pltpu.make_async_remote_copy(
        src_ref=xin.at[core], dst_ref=xin.at[core], send_sem=xs_send, recv_sem=xs_recv,
        device_id=(ep, sib), device_id_type=MESH,
    )
    from_sib = pltpu.make_async_remote_copy(
        src_ref=xin.at[1 - core], dst_ref=xin.at[1 - core], send_sem=xs_send, recv_sem=xs_recv,
        device_id=(ep, sib), device_id_type=MESH,
    )
    to_sib.start()
    from_sib.wait_recv()

    @pl.loop(0, 2 * (NEP // 2))
    def _(i):
        half = i // (NEP // 2)
        pair = lax.rem(i, NEP // 2)
        two = xin[half, pl.ds(pair * 2, 2)].astype(F32).reshape(2 * CAP, DM)
        xmat[half, pl.ds(pl.multiple_of(pair * 2 * CAP, 16), 2 * CAP), :] = two.astype(BF16)

    def hidden(origin):
        @pl.loop(0, 2)
        def _(half):
            both = jnp.concatenate([gbuf[origin], ubuf[origin]], axis=1)
            pre = jnp.dot(xmat[half], both, preferred_element_type=F32)
            gate = jnp.minimum(pre[:, :SHARD], 7.0)
            up = jnp.clip(pre[:, SHARD:], -7.0, 7.0)
            units[half, origin] = ((up + 1.0) * gate * jax.nn.sigmoid(1.702 * gate)).astype(BF16)

    def hidden_pair(hop):
        @pl.loop(0, 2)
        def _(d):
            hidden(lax.rem(z + jnp.where(d == 0, NZ - hop, hop), NZ))

    hidden(z)
    hidden_pair(1)
    forward(gu, 2)
    hidden_pair(2)
    forward(gu, 3)
    loads[4].wait()
    start(dn, 1)
    hidden_pair(3)

    arrive(gu)
    hidden(lax.rem(z + 4, NZ))

    def down(k, half):
        lo = sum(DCS[:k])
        left = jnp.concatenate([units[half, o] for o in range(NZ)], axis=1)
        right = jnp.concatenate([dbuf[o, lo : lo + DCS[k], :] for o in range(NZ)], axis=1)
        return lax.dot_general(left, right, (((1,), (1,)), ((), ())), preferred_element_type=F32)

    def partial_copy(k):
        return pltpu.make_async_remote_copy(
            src_ref=ps[k], dst_ref=pr[k], send_sem=ps_send.at[k], recv_sem=ps_recv.at[k],
            device_id=(ep, sib), device_id_type=MESH,
        )

    def back(k, peer, src):
        return pltpu.make_async_remote_copy(
            src_ref=rs[k].at[peer], dst_ref=rb[k].at[src],
            send_sem=rt_send.at[k, peer], recv_sem=rt_recv.at[k, src],
            device_id=(peer, tp), device_id_type=MESH,
        )

    def stage1(k):
        ps[k][...] = down(k, 1 - core).astype(BF16)
        partial_copy(k).start()
        acc[k][...] = down(k, core)

    def stage2(k):
        partial_copy(k).wait_recv()
        total = acc[k][...] + pr[k][...].astype(F32)
        rs[k][...] = total.reshape(NEP, CAP, DCS[k]).astype(BF16)

        @pl.loop(1, NEP)
        def _(j):
            back(k, lax.rem(ep + j, NEP), ep).start()

        rb[k][ep] = rs[k][ep]

    def out_copy(k):
        cols = pl.ds(sum(DCS[:k]), DCS[k])
        return pltpu.make_async_copy(out_buf.at[:, cols], out_ref.at[:, cols], out_sem.at[k])

    def stage3(k):
        @pl.loop(1, NEP)
        def _(j):
            src = lax.rem(ep + j, NEP)
            back(k, src, src).wait_recv()

        got = rb[k][...].astype(F32).reshape(ROWS, DCS[k]).astype(BF16)
        mixed = jnp.dot(comb[0], got, preferred_element_type=F32)
        mixed = mixed + jnp.dot(comb[1], got, preferred_element_type=F32)
        out_buf[:, sum(DCS[:k]) : sum(DCS[: k + 1])] = mixed.astype(BF16)
        out_copy(k).start()

    for i in range(NDC + 6):
        if i < NDC:
            forward(dn[i : i + 1], 1)
        if 0 <= i - 1 < NDC:
            forward(dn[i - 1 : i], 2)
        if 0 <= i - 2 < NDC:
            forward(dn[i - 2 : i - 1], 3)
        if i - 2 == NDC - 1:
            @pl.loop(1, NEP)
            def _(k):
                hand(lax.rem(tp + k, NEP), tp).start()

        if 0 <= i - 4 < NDC:
            stage2(i - 4)
        if 0 <= i - 3 < NDC:
            arrive(dn[i - 3 : i - 2])
            stage1(i - 3)
        if 0 <= i - 6 < NDC - 1:
            stage3(i - 6)
        if i - 6 == NDC - 2:
            loads[6].wait()

            @pl.loop(1, NEP)
            def _(k):
                src = lax.rem(tp + k, NEP)
                hand(src, src).wait_recv()

            hidden_rows = mix_in[...].reshape(NEP * CH, SHARD).astype(F32).T.astype(BF16)

            @pl.loop(0, 4)
            def _(k):
                cols = pl.ds(pl.multiple_of(k * 512, 512), 512)
                scan_out[:, cols] = jnp.dot(hidden_rows, map_ref[:, cols], preferred_element_type=F32).astype(BF16)

            scan_copy = pltpu.make_async_copy(scan_out, scan_ref, out_sem.at[NDC])
            scan_copy.start()
        if i - 6 == NDC - 1:
            stage3(NDC - 1)

    for p in gu + dn:
        for d in (0, 1):
            for hop in (1, 2, 3, 4):
                ring(d, hop, p, sent(d, hop)).wait_send()

    @pl.loop(1, NEP)
    def _(k):
        peer = lax.rem(ep + k, NEP)
        dispatch(peer, ep).wait_send()
        for c in range(NDC):
            back(c, peer, ep).wait_send()

    @pl.loop(1, NEP)
    def _(k):
        total(lax.rem(ep + k, NEP), ep).wait_send()
        hand(lax.rem(tp + k, NEP), tp).wait_send()

    scan_copy.wait()
    for k in range(NDC):
        out_copy(k).wait()
    halo.wait_send()
    to_sib.wait_send()
    for k in range(NDC):
        partial_copy(k).wait_send()


def on_device(
    scan_source_values,
    switch_path_values,
    causal_filter_coefficients,
    scan_switch_blockmap,
    entry_switch_blockmap,
    feature_fading_speeds,
    spike_amount,
    final_linear_map,
    dispatched_group_activity,
    specialist_rmsgain,
    selected_specialist_ids,
    selected_specialist_share,
    specialist_switch_maps,
    specialist_widen_maps,
    specialist_shrink_maps,
):
    hbm = pl.BlockSpec(memory_space=pltpu.HBM)
    dma = pltpu.SemaphoreType.DMA
    result = jax.ShapeDtypeStruct((SHARD, DM), BF16)
    computed = pl.pallas_call(
        whole_kernel,
        out_shape=(result, result),
        in_specs=[hbm] * 15,
        out_specs=(hbm, hbm),
        scratch_shapes=[
            pltpu.VMEM((NZ, DM, SHARD), BF16),
            pltpu.VMEM((NZ, DM, SHARD), BF16),
            pltpu.VMEM((NZ, DM, SHARD), BF16),
            pltpu.VMEM((NEP, CAP, DM), BF16),
            pltpu.VMEM((2, NEP, CAP, DM), BF16),
            pltpu.VMEM((2, ROWS, DM), BF16),
            pltpu.VMEM((2, NZ, ROWS, SHARD), BF16),
            tuple(pltpu.VMEM((ROWS, w), F32) for w in DCS),
            tuple(pltpu.VMEM((ROWS, w), BF16) for w in DCS),
            tuple(pltpu.VMEM((ROWS, w), BF16) for w in DCS),
            tuple(pltpu.VMEM((NEP, CAP, w), BF16) for w in DCS),
            tuple(pltpu.VMEM((NEP, CAP, w), BF16) for w in DCS),
            pltpu.VMEM((2, SHARD, ROWS), BF16),
            pltpu.VMEM((NEP, SHARD), BF16),
            pltpu.VMEM((2, SHARD), jnp.int32),
            pltpu.VMEM((2, SHARD), F32),
            pltpu.VMEM((4, NZ * SHARD), BF16),
            pltpu.VMEM((CH, CH), BF16),
            pltpu.VMEM((CH, CH), BF16),
            pltpu.VMEM((NZ, SHARD), F32),
            pltpu.VMEM((1, POS), F32),
            pltpu.VMEM((SHARD, DM), BF16),
            pltpu.VMEM((CH, HALO + POS), BF16),
            pltpu.VMEM((CH, POS), BF16),
            pltpu.VMEM((NEP * CH, DM), BF16),
            pltpu.VMEM((CH, POS), F32),
            pltpu.VMEM((CH, POS), F32),
            pltpu.VMEM((8, SHARD), F32),
            pltpu.VMEM((NEP, 8, SHARD), F32),
            pltpu.VMEM((NEP, CH, SHARD), BF16),
            pltpu.VMEM((NEP, CH, SHARD), BF16),
            dma((2, 4, NG + NDC)), dma((2, 4, NG + NDC)),
            dma((NEP,)), dma((NEP,)),
            dma, dma,
            dma((NDC,)), dma((NDC,)),
            dma((NDC, NEP)), dma((NDC, NEP)),
            pltpu.VMEM((SHARD, DM), BF16),
            pltpu.VMEM((SHARD, DM), BF16),
            dma((15,)), dma((NDC + 1,)), dma, dma,
            dma((NEP,)), dma((NEP,)),
            dma((NEP,)), dma((NEP,)),
        ],
        compiler_params=pltpu.CompilerParams(
            collective_id=0, has_side_effects=True, vmem_limit_bytes=62 * 2**20
        ),
    )(
        specialist_rmsgain.reshape(NEP, SHARD),
        selected_specialist_ids.T,
        selected_specialist_share.T,
        causal_filter_coefficients.T,
        scan_switch_blockmap,
        entry_switch_blockmap,
        feature_fading_speeds.reshape(8, SHARD),
        spike_amount.reshape(1, POS),
        scan_source_values,
        switch_path_values,
        final_linear_map,
        dispatched_group_activity,
        specialist_switch_maps[0],
        specialist_widen_maps[0],
        specialist_shrink_maps[0],
    )
    return pl.pallas_call(
        handover_kernel,
        out_shape=(result, result),
        in_specs=[hbm] * 2,
        out_specs=(hbm, hbm),
        scratch_shapes=[pltpu.VMEM((4, SHARD // 2, DM), BF16), dma((4,)), dma((4,))],
    )(*computed)


def handover_kernel(scan_in, moe_in, scan_ref, moe_ref, stage, in_sem, out_sem):
    half = SHARD // 2
    parts = [(a, b, pl.ds(h * half, half)) for a, b in ((scan_in, scan_ref), (moe_in, moe_ref)) for h in (0, 1)]
    ins = [pltpu.make_async_copy(a.at[r], stage.at[i], in_sem.at[i]) for i, (a, b, r) in enumerate(parts)]
    outs = [pltpu.make_async_copy(stage.at[i], b.at[r], out_sem.at[i]) for i, (a, b, r) in enumerate(parts)]
    for copy in ins:
        copy.start()
    for i in range(4):
        ins[i].wait()
        outs[i].start()
    for copy in outs:
        copy.wait()


def solution(mesh):
    in_specs = (
        P("tp", "ep"),
        P("tp", "ep"),
        P(),
        P(),
        P(),
        P(),
        P("ep"),
        P(),
        P(("ep", "tp"), None),
        P(),
        P(("ep", "tp"), None),
        P(("ep", "tp"), None),
        P("ep", None, "tp"),
        P("ep", None, "tp"),
        P("ep", None, "tp"),
    )
    out_specs = (P(("ep", "tp"), None), P(("ep", "tp"), None))
    return jax.shard_map(
        on_device, mesh=mesh, in_specs=in_specs, out_specs=out_specs, check_vma=False
    )
```
